32 devices in a mesh: fs: 16 (over z, y, x), tp: 2 (over core).
Axes of the slice: x: 2, y: 2, z: 4, core: 2. Of those that a mesh axis runs over, the one named last changes fastest.
Arguments:
- tokens: bfloat16 [12288, 2048], P('fs'), may hold values from -6 to 6
- norm_gain: float32 [2048], replicated, may hold values from 0.1 to 1.9
- gate_weight: float32 [2048, 5632], P('fs', 'tp'), may hold values from -0.125 to 0.125
- up_weight: float32 [2048, 5632], P('fs', 'tp'), may hold values from -0.125 to 0.125
- gate_scale: float32 [5632], P('tp'), may hold values from 0.1 to 1.9
- up_scale: float32 [5632], P('tp'), may hold values from 0.1 to 1.9
- down_weight: float32 [5632, 2048], P('tp', 'fs'), may hold values from -0.078125 to 0.078125
- down_scale: float32 [2048], P('tp'), may hold values from 0.1 to 1.9
Outputs:
- mixed: bfloat16 [12288, 2048], P('fs', 'tp')
The draws below stay inside these ranges and needn't reach their ends.
All inputs are finite; a program needn't handle non-finite values.
Results may differ from the reference program's by a relative error of at most 0.014.
Values may be sent and summed in bfloat16 or wider, within the bound.
A program may use at most 128 MiB of HBM per device.

```python
import jax
import jax.numpy as jnp
from jax import lax

D = 2048
FF = 5632
TOK_DEV = 768
TOKENS = 12288
N_FS = 16
N_TP = 2


def level_of(key, shape, cuts, low, high):
    loudness, own = 1.0, jax.random.fold_in(key, 6)
    for position, shards_of in cuts:
        draws = jnp.exp(jax.random.uniform(jax.random.fold_in(own, position), (shards_of,), jnp.float32, low / len(cuts), high / len(cuts)))
        loudness = loudness * jnp.repeat(draws, shape[position] // shards_of).reshape([-1 if axis == position else 1 for axis in range(len(shape))])
    return loudness


def centred(own_key, dims, spread, most, split=(), held_as=jnp.bfloat16):
    drawn = spread * jax.random.normal(own_key, dims, jnp.float32)
    if split:
        drawn = drawn * level_of(own_key, dims, split, -0.22, 0.18)
    return jnp.clip(drawn, -most, most).astype(held_as)


def setup_inputs(seed: int = 0) -> dict:
    arg_keys = jax.random.split(jax.random.key(seed), 9)
    return {
        "tokens": centred(arg_keys[0], (TOKENS, D), 1.0, 6.0, ((0, 16),)),
        "norm_gain": jnp.clip(1.0 + 0.18 * jax.random.normal(arg_keys[1], (D,), jnp.float32), 0.1, 1.9),
        "gate_weight": centred(arg_keys[2], (D, FF), D ** -0.5, 0.125, ((0, 16), (1, 2)), jnp.float32),
        "up_weight": centred(arg_keys[3], (D, FF), D ** -0.5, 0.125, ((0, 16), (1, 2)), jnp.float32),
        "gate_scale": jnp.clip(1.0 + 0.18 * jax.random.normal(arg_keys[4], (FF,), jnp.float32), 0.1, 1.9),
        "up_scale": jnp.clip(1.0 + 0.18 * jax.random.normal(arg_keys[5], (FF,), jnp.float32), 0.1, 1.9),
        "down_weight": centred(arg_keys[6], (FF, D), FF ** -0.5, 0.078125, ((0, 2), (1, 16)), jnp.float32),
        "down_scale": jnp.clip(1.0 + 0.18 * jax.random.normal(arg_keys[7], (D,), jnp.float32), 0.1, 1.9),
    }


def reference(tokens, norm_gain, gate_weight, up_weight, gate_scale, up_scale, down_weight, down_scale):
    gate_low = gate_weight.astype(jnp.bfloat16)
    up_low = up_weight.astype(jnp.bfloat16)
    down_low = down_weight.astype(jnp.bfloat16).reshape(N_TP, FF // N_TP, D)

    def one_block(rows):
        values = rows.astype(jnp.float32)
        normed = (values * lax.rsqrt(lax.optimization_barrier(jnp.mean(values * values, axis=-1, keepdims=True)) + 1e-06) * norm_gain).astype(jnp.bfloat16)
        gate = jnp.dot(normed, gate_low, preferred_element_type=jnp.float32) * gate_scale
        up = jnp.dot(normed, up_low, preferred_element_type=jnp.float32) * up_scale
        hidden = (jax.nn.silu(gate) * up).astype(jnp.bfloat16).reshape(rows.shape[0], N_TP, FF // N_TP)
        total = jnp.zeros((rows.shape[0], D), jnp.float32)
        for block in range(N_TP):
            partial_sum = jnp.dot(hidden[:, block], down_low[block], preferred_element_type=jnp.float32).astype(jnp.bfloat16)
            partial_sum = lax.optimization_barrier(partial_sum)
            total = total + partial_sum.astype(jnp.float32)
        return (total * down_scale).astype(jnp.bfloat16)
    blocks = lax.map(one_block, tokens.reshape(N_FS, TOK_DEV, D))
    return blocks.reshape(TOKENS, D)
```

```python
import jax
import jax.numpy as jnp
from jax import lax
from jax.experimental import pallas as pl
from jax.experimental.pallas import tpu as pltpu
from jax.sharding import PartitionSpec as P

MESH = pl.DeviceIdType.MESH
NT = (((1,), (1,)), ((), ()))
NN = (((1,), (0,)), ((), ()))


def norm(tokens, norm_gain):
    values = tokens.astype(jnp.float32)
    return (
        values * lax.rsqrt(jnp.mean(values * values, axis=-1, keepdims=True) + 1e-06) * norm_gain
    ).astype(jnp.bfloat16)


def gathered(tokens, norm_gain, gate_weight, up_weight, gate_scale, up_scale, down_weight, down_scale):
    normed = norm(tokens, norm_gain)

    def add_rows(piece):
        return jnp.dot(normed, piece, preferred_element_type=jnp.float32)

    gate = add_rows(lax.all_gather(gate_weight.astype(jnp.bfloat16), "fs", axis=0, tiled=True))
    up = add_rows(lax.all_gather(up_weight.astype(jnp.bfloat16), "fs", axis=0, tiled=True))
    hidden = (jax.nn.silu(gate * gate_scale) * (up * up_scale)).astype(jnp.bfloat16)
    terms = jnp.dot(
        hidden,
        lax.all_gather(down_weight.astype(jnp.bfloat16), "fs", axis=1, tiled=True),
        preferred_element_type=jnp.float32,
    )
    summed = lax.psum_scatter(
        terms.astype(jnp.bfloat16), "tp", scatter_dimension=1, tiled=True
    ).astype(jnp.float32)
    return (summed * down_scale).astype(jnp.bfloat16)


def kernel(
    gu_ref, d_ref, xn_ref, gs_ref, us_ref, ds_ref, out_ref,
    xbuf, wgu, wd, accg, accu, hid, pbuf, rbuf,
    lw_sem, lx_sem, rsh_send, rsh_recv, x_send, x_recv, xf_send, xf_recv,
    z_send, z_recv, p_send, p_recv, r_send, r_recv,
):
    f, c = lax.axis_index("fs"), lax.axis_index("tp")
    z, q = lax.div(f, 4), lax.rem(f, 4)
    qk = [q, q + 1 - 2 * lax.rem(q, 2), lax.rem(q + 2, 4), 3 - q]
    part = wd.shape[1]
    width = 4 * wd.shape[2]
    rows = xn_ref.shape[0]
    half = rows // 2
    tile = rows // 3
    tiles = rows // tile
    partner = (f, 1 - c)

    def at(k):
        return (4 * z + qk[k], c)

    def rcopy(src, dst, ssem, rsem, dev):
        return pltpu.make_async_remote_copy(
            src_ref=src, dst_ref=dst, send_sem=ssem, recv_sem=rsem,
            device_id=dev, device_id_type=MESH,
        )

    barrier = pltpu.get_barrier_semaphore()

    def greet(dev):
        pl.semaphore_signal(barrier, inc=1, device_id=dev, device_id_type=MESH)

    greet(partner)
    for k in (1, 2, 3):
        greet(at(k))
    pl.when(z > 0)(lambda: greet((f - 4, c)))
    pl.when(z < 3)(lambda: greet((f + 4, c)))

    slot = [wgu, wd]

    def stored(cls, k):
        cut = pl.ds(pl.multiple_of(qk[k] * part, 16), part)
        return gu_ref.at[:, cut, :] if cls == 0 else d_ref.at[cut, :]

    def own(cls):
        return pltpu.make_async_copy(stored(cls, 0), slot[cls].at[f], lw_sem.at[cls])

    def rsh(cls, k, landing):
        return rcopy(
            stored(cls, k), slot[cls].at[landing],
            rsh_send.at[cls, k - 1], rsh_recv.at[cls, k - 1], at(k),
        )

    mine = pl.ds(pl.multiple_of(half * c, 16), half)
    theirs = pl.ds(pl.multiple_of(half * (1 - c), 16), half)

    def xcopy(k, landing):
        return rcopy(
            xn_ref.at[mine, :], xbuf.at[landing, mine, :],
            x_send.at[k - 1], x_recv.at[k - 1], at(k),
        )

    def xshare(k, cut):
        return rcopy(
            xbuf.at[qk[k], mine, :], xbuf.at[qk[k], cut, :],
            xf_send.at[k - 1], xf_recv.at[k - 1], partner,
        )

    local_x = pltpu.make_async_copy(xn_ref, xbuf.at[q], lx_sem)

    def zcopy(cls, i, d):
        dev = (f + 4, c) if d == 0 else (f - 4, c)
        return rcopy(slot[cls].at[i], slot[cls].at[i], z_send.at[d, cls, i], z_recv.at[cls, i], dev)

    def up_down(cls, i):
        pl.when(z < 3)(lambda: zcopy(cls, i, 0).start())
        pl.when(z > 0)(lambda: zcopy(cls, i, 1).start())

    def relay(cls, r):
        for k in range(4):
            low = 4 * (z - r) + qk[k]
            high = 4 * (z + r) + qk[k]

            @pl.when(z >= r)
            def _():
                zcopy(cls, low, 0).wait_recv()
                if r < 3:
                    pl.when(z < 3)(lambda: zcopy(cls, low, 0).start())

            @pl.when(z + r <= 3)
            def _():
                zcopy(cls, high, 1).wait_recv()
                if r < 3:
                    pl.when(z > 0)(lambda: zcopy(cls, high, 1).start())

    own(0).start()
    own(1).start()
    local_x.start()
    pl.semaphore_wait(barrier, 4 + jnp.minimum(z, 1) + jnp.minimum(3 - z, 1))

    for cls in (0, 1):
        for k in (1, 2, 3):
            rsh(cls, k, f).start()
    for k in (1, 2, 3):
        xcopy(k, q).start()
    own(0).wait()
    up_down(0, f)
    for k in (1, 2, 3):
        rsh(0, k, 4 * z + qk[k]).wait_recv()
        up_down(0, 4 * z + qk[k])
    relay(0, 1)
    relay(0, 2)
    own(1).wait()
    up_down(1, f)
    for k in (1, 2, 3):
        rsh(1, k, 4 * z + qk[k]).wait_recv()
        up_down(1, 4 * z + qk[k])
    for k in (1, 2, 3):
        xcopy(k, qk[k]).wait_recv()
        xshare(k, mine).start()
    local_x.wait()
    relay(1, 1)
    for k in (1, 2, 3):
        xshare(k, theirs).wait_recv()

    side = lax.div(z, 2)
    zz = z + side * (3 - 2 * z)

    def turn(t):
        base = t if t >= 2 else lax.rem(t + zz, 2)
        return base + side * (3 - 2 * base)

    def columns(s):
        return pl.ds(pl.multiple_of(s * width, 128), width)

    def gate_up(t):
        s = turn(t)

        def step(m, _):
            there = pl.ds(pl.multiple_of(lax.rem(m, tiles) * tile, 16), tile)
            here = pl.ds(pl.multiple_of(m * tile, 16), tile)
            x = xbuf[lax.div(m, tiles), there, columns(s)]
            found = []
            for j, acc in enumerate((accg, accu)):
                w = jnp.concatenate([wgu[4 * s + k, j] for k in range(4)], axis=1)
                part_sum = lax.dot_general(x, w, NT, preferred_element_type=jnp.float32)
                if t > 0:
                    part_sum = part_sum + acc[here, :]
                if t < 3:
                    acc[here, :] = part_sum
                found.append(part_sum)
            if t == 3:
                g = found[0] * gs_ref[...]
                u = found[1] * us_ref[...]
                hid[here, :] = (g / (1.0 + jnp.exp(-g)) * u).astype(jnp.bfloat16)
            return 0

        lax.fori_loop(0, 4 * tiles, step, 0)

    gate_up(0)
    gate_up(1)
    relay(1, 2)
    gate_up(2)
    relay(0, 3)
    gate_up(3)
    for k in (1, 2, 3):
        xshare(k, mine).wait_send()

    order = (3, 1, 2, 0)

    def pcopy(s, k):
        i = lax.rem(s, 2)
        return rcopy(
            xbuf.at[qk[k], :, columns(s)], pbuf.at[i, qk[k]],
            p_send.at[i, qk[k]], p_recv.at[i, qk[k]], partner,
        )

    def scopy(s, k):
        i = lax.rem(s, 2)
        return rcopy(
            xbuf.at[qk[k], :, columns(s)], rbuf.at[i, k - 1],
            r_send.at[i, k - 1], r_recv.at[i, k - 1], at(k),
        )

    def finish(s, k):
        @pl.when(lax.div(s, 2) == c)
        def _():
            pcopy(s, k).wait_recv()

            def step(m, _):
                here = pl.ds(pl.multiple_of(m * tile, 16), tile)
                both = xbuf[qk[k], here, columns(s)].astype(jnp.float32) + pbuf[
                    lax.rem(s, 2), qk[k], here, :
                ].astype(jnp.float32)
                xbuf[qk[k], here, columns(s)] = both.astype(jnp.bfloat16)
                return 0

            lax.fori_loop(0, tiles, step, 0)
            if k:
                scopy(s, k).start()

    def down(t):
        s = turn(t)
        for n, k in enumerate(order):
            def step(m, _):
                here = pl.ds(pl.multiple_of(m * tile, 16), tile)
                h = hid[pl.ds(pl.multiple_of(qk[k] * rows + m * tile, 16), tile), :]
                w = jnp.concatenate([wd[4 * s + j] for j in range(4)], axis=1)
                o = lax.dot_general(h, w, NN, preferred_element_type=jnp.float32)
                xbuf[qk[k], here, columns(s)] = o.astype(jnp.bfloat16)
                return 0

            lax.fori_loop(0, tiles, step, 0)
            pl.when(lax.div(s, 2) != c)(lambda: pcopy(s, k).start())
            if n:
                finish(s, order[n - 1])
        finish(s, order[-1])

    down(0)
    down(1)
    down(2)
    relay(1, 3)
    down(3)

    for i in range(2):
        s = 2 * c + i
        for k in (1, 2, 3):
            scopy(s, k).wait_recv()

        def step(m, _):
            here = pl.ds(pl.multiple_of(m * tile, 16), tile)
            total = xbuf[q, here, columns(s)].astype(jnp.float32)
            for k in range(3):
                total = total + rbuf[i, k, here, :].astype(jnp.float32)
            cols = slice(i * width, (i + 1) * width)
            out_ref[here, cols] = (total * ds_ref[:, cols]).astype(jnp.bfloat16)
            return 0

        lax.fori_loop(0, tiles, step, 0)

    for cls in (0, 1):
        for k in (1, 2, 3):
            rsh(cls, k, f).wait_send()
        for r in range(3):
            for k in range(4):
                low, high = 4 * (z - r) + qk[k], 4 * (z + r) + qk[k]
                pl.when((z >= r) & (z < 3))(lambda: zcopy(cls, low, 0).wait_send())
                pl.when((z + r <= 3) & (z > 0))(lambda: zcopy(cls, high, 1).wait_send())
    for k in (1, 2, 3):
        xcopy(k, q).wait_send()
    for i in range(2):
        for k in range(4):
            pcopy(2 * (1 - c) + i, k).wait_send()
            if k:
                scopy(2 * c + i, k).wait_send()


def planes(tokens, norm_gain, gate_weight, up_weight, gate_scale, up_scale, down_weight, down_scale):
    rows, model = tokens.shape
    block, units = gate_weight.shape
    part, width = units // 4, 4 * block
    normed = norm(tokens, norm_gain)
    gu = jnp.stack([gate_weight.astype(jnp.bfloat16).T, up_weight.astype(jnp.bfloat16).T])
    low = down_weight.astype(jnp.bfloat16)
    first = lax.rem(lax.axis_index("fs"), 4) * part
    gs = lax.dynamic_slice(gate_scale, (first,), (part,))[None]
    us = lax.dynamic_slice(up_scale, (first,), (part,))[None]
    bf, f32, dma = jnp.bfloat16, jnp.float32, pltpu.SemaphoreType.DMA
    hbm = pl.BlockSpec(memory_space=pl.ANY)
    vmem = pl.BlockSpec(memory_space=pltpu.VMEM)
    return pl.pallas_call(
        kernel,
        out_shape=jax.ShapeDtypeStruct((rows, down_scale.shape[0]), bf),
        in_specs=[hbm, hbm, hbm, vmem, vmem, vmem],
        out_specs=vmem,
        scratch_shapes=[
            pltpu.VMEM((4, rows, model), bf),
            pltpu.VMEM((16, 2, part, block), bf),
            pltpu.VMEM((16, part, block), bf),
            pltpu.VMEM((4 * rows, part), f32),
            pltpu.VMEM((4 * rows, part), f32),
            pltpu.VMEM((4 * rows, part), bf),
            pltpu.VMEM((2, 4, rows, width), bf),
            pltpu.VMEM((2, 3, rows, width), bf),
            dma((2,)), dma, dma((2, 3)), dma((2, 3)),
            dma((3,)), dma((3,)), dma((3,)), dma((3,)),
            dma((2, 2, 16)), dma((2, 16)),
            dma((2, 4)), dma((2, 4)), dma((2, 3)), dma((2, 3)),
        ],
        compiler_params=pltpu.CompilerParams(
            collective_id=0, has_side_effects=True, vmem_limit_bytes=67043328
        ),
    )(gu, low, normed, gs, us, down_scale[None])


def solution(mesh):
    in_specs = (
        P("fs", None),
        P(),
        P("fs", "tp"),
        P("fs", "tp"),
        P("tp"),
        P("tp"),
        P("tp", "fs"),
        P("tp"),
    )
    out_specs = P("fs", "tp")
    body = planes if (mesh.shape["fs"], mesh.shape["tp"]) == (16, 2) else gathered
    return jax.shard_map(body, mesh=mesh, in_specs=in_specs, out_specs=out_specs, check_vma=False)
```

```python
import jax
import jax.numpy as jnp
from jax import lax
from jax.experimental import pallas as pl
from jax.experimental.pallas import tpu as pltpu
from jax.sharding import PartitionSpec as P

MESH = pl.DeviceIdType.MESH
NT = (((1,), (1,)), ((), ()))
NN = (((1,), (0,)), ((), ()))


def norm(tokens, norm_gain):
    values = tokens.astype(jnp.float32)
    return (
        values * lax.rsqrt(jnp.mean(values * values, axis=-1, keepdims=True) + 1e-06) * norm_gain
    ).astype(jnp.bfloat16)


def gathered(tokens, norm_gain, gate_weight, up_weight, gate_scale, up_scale, down_weight, down_scale):
    normed = norm(tokens, norm_gain)

    def add_rows(piece):
        return jnp.dot(normed, piece, preferred_element_type=jnp.float32)

    gate = add_rows(lax.all_gather(gate_weight.astype(jnp.bfloat16), "fs", axis=0, tiled=True))
    up = add_rows(lax.all_gather(up_weight.astype(jnp.bfloat16), "fs", axis=0, tiled=True))
    hidden = (jax.nn.silu(gate * gate_scale) * (up * up_scale)).astype(jnp.bfloat16)
    terms = jnp.dot(
        hidden,
        lax.all_gather(down_weight.astype(jnp.bfloat16), "fs", axis=1, tiled=True),
        preferred_element_type=jnp.float32,
    )
    summed = lax.psum_scatter(
        terms.astype(jnp.bfloat16), "tp", scatter_dimension=1, tiled=True
    ).astype(jnp.float32)
    return (summed * down_scale).astype(jnp.bfloat16)


def kernel(
    gu_ref, d_ref, xn_ref, gs_ref, us_ref, ds_ref, out_ref,
    xbuf, wgu, wd, accg, accu, hid, pbuf, rbuf,
    lw_sem, lx_sem, rsh_send, rsh_recv, x_send, x_recv, f_send, f_recv, xf_send, xf_recv,
    z_send, z_recv, p_send, p_recv, r_send, r_recv,
):
    f, c = lax.axis_index("fs"), lax.axis_index("tp")
    z, q = lax.div(f, 4), lax.rem(f, 4)
    qk = [q, q + 1 - 2 * lax.rem(q, 2), lax.rem(q + 2, 4), 3 - q]
    part = wd.shape[1]
    width = 4 * wd.shape[2]
    rows = xn_ref.shape[0]
    half = rows // 2
    quarter = half // 2
    tile = rows // 3
    tiles = rows // tile
    partner = (f, 1 - c)

    def at(k):
        return (4 * z + qk[k], c)

    def rcopy(src, dst, ssem, rsem, dev):
        return pltpu.make_async_remote_copy(
            src_ref=src, dst_ref=dst, send_sem=ssem, recv_sem=rsem,
            device_id=dev, device_id_type=MESH,
        )

    barrier = pltpu.get_barrier_semaphore()

    def greet(dev):
        pl.semaphore_signal(barrier, inc=1, device_id=dev, device_id_type=MESH)

    greet(partner)
    for k in (1, 2, 3):
        greet(at(k))
    pl.when(z > 0)(lambda: greet((f - 4, c)))
    pl.when(z < 3)(lambda: greet((f + 4, c)))

    slot = [wgu, wd]

    def stored(cls, k):
        units = pl.ds(pl.multiple_of(qk[k] * part, 16), part)
        return gu_ref.at[:, units, :] if cls == 0 else d_ref.at[units, :]

    def own(cls):
        return pltpu.make_async_copy(stored(cls, 0), slot[cls].at[f], lw_sem.at[cls])

    def rsh(cls, k, landing):
        return rcopy(
            stored(cls, k), slot[cls].at[landing],
            rsh_send.at[cls, k - 1], rsh_recv.at[cls, k - 1], at(k),
        )

    def cut(core, p):
        return pl.ds(pl.multiple_of(half * core + quarter * p, 16), quarter)

    def xcopy(k, p, landing):
        return rcopy(
            xn_ref.at[cut(c, p), :], xbuf.at[landing, cut(c, p), :],
            x_send.at[k - 1, p], x_recv.at[k - 1, p], at(k),
        )

    def fcopy(p, k):
        return rcopy(
            xbuf.at[qk[k], cut(c, p), :], xbuf.at[qk[k], cut(c, p), :],
            f_send.at[p], f_recv.at[p], at(2 - p),
        )

    def xshare(k, p, core):
        return rcopy(
            xbuf.at[qk[k], cut(core, p), :], xbuf.at[qk[k], cut(core, p), :],
            xf_send.at[k - 1, p], xf_recv.at[k - 1, p], partner,
        )

    local_x = pltpu.make_async_copy(xn_ref, xbuf.at[q], lx_sem)

    def zcopy(cls, i, d):
        dev = (f + 4, c) if d == 0 else (f - 4, c)
        return rcopy(slot[cls].at[i], slot[cls].at[i], z_send.at[d, cls, i], z_recv.at[cls, i], dev)

    def up_down(cls, i):
        pl.when(z < 3)(lambda: zcopy(cls, i, 0).start())
        pl.when(z > 0)(lambda: zcopy(cls, i, 1).start())

    def relay(cls, r):
        for k in range(4):
            low = 4 * (z - r) + qk[k]
            high = 4 * (z + r) + qk[k]

            @pl.when(z >= r)
            def _():
                zcopy(cls, low, 0).wait_recv()
                if r < 3:
                    pl.when(z < 3)(lambda: zcopy(cls, low, 0).start())

            @pl.when(z + r <= 3)
            def _():
                zcopy(cls, high, 1).wait_recv()
                if r < 3:
                    pl.when(z > 0)(lambda: zcopy(cls, high, 1).start())

    own(0).start()
    own(1).start()
    local_x.start()
    pl.semaphore_wait(barrier, 4 + jnp.minimum(z, 1) + jnp.minimum(3 - z, 1))

    for cls in (0, 1):
        for k in (1, 2, 3):
            rsh(cls, k, f).start()
    for k, p in ((1, 0), (2, 1), (1, 1), (2, 0)):
        xcopy(k, p, q).start()
    own(0).wait()
    up_down(0, f)
    for k in (1, 2, 3):
        rsh(0, k, 4 * z + qk[k]).wait_recv()
        up_down(0, 4 * z + qk[k])
    relay(0, 1)
    for p in (0, 1):
        xcopy(1 + p, p, qk[1 + p]).wait_recv()
        fcopy(p, 1 + p).start()
        xshare(1 + p, p, c).start()
    relay(0, 2)
    own(1).wait()
    up_down(1, f)
    for k in (1, 2, 3):
        rsh(1, k, 4 * z + qk[k]).wait_recv()
        up_down(1, 4 * z + qk[k])
    for p in (0, 1):
        xcopy(2 - p, p, qk[2 - p]).wait_recv()
        xshare(2 - p, p, c).start()
    local_x.wait()
    relay(1, 1)
    for p in (0, 1):
        fcopy(p, 3).wait_recv()
        xshare(3, p, c).start()
    for k in (1, 2, 3):
        for p in (0, 1):
            xshare(k, p, 1 - c).wait_recv()

    side = lax.div(z, 2)
    zz = z + side * (3 - 2 * z)

    def turn(t):
        base = t if t >= 2 else lax.rem(t + zz, 2)
        return base + side * (3 - 2 * base)

    def columns(s):
        return pl.ds(pl.multiple_of(s * width, 128), width)

    def gate_up(t):
        s = turn(t)

        def step(m, _):
            there = pl.ds(pl.multiple_of(lax.rem(m, tiles) * tile, 16), tile)
            here = pl.ds(pl.multiple_of(m * tile, 16), tile)
            x = xbuf[lax.div(m, tiles), there, columns(s)]
            found = []
            for j, acc in enumerate((accg, accu)):
                w = jnp.concatenate([wgu[4 * s + k, j] for k in range(4)], axis=1)
                part_sum = lax.dot_general(x, w, NT, preferred_element_type=jnp.float32)
                if t > 0:
                    part_sum = part_sum + acc[here, :]
                if t < 3:
                    acc[here, :] = part_sum
                found.append(part_sum)
            if t == 3:
                g = found[0] * gs_ref[...]
                u = found[1] * us_ref[...]
                hid[here, :] = (g / (1.0 + jnp.exp(-g)) * u).astype(jnp.bfloat16)
            return 0

        lax.fori_loop(0, 4 * tiles, step, 0)

    gate_up(0)
    gate_up(1)
    relay(1, 2)
    gate_up(2)
    relay(0, 3)
    gate_up(3)
    for p in (0, 1):
        fcopy(p, 1 + p).wait_send()
        for k in (1, 2, 3):
            xshare(k, p, c).wait_send()

    order = (3, 1, 2, 0)

    def pcopy(s, k):
        i = lax.rem(s, 2)
        return rcopy(
            xbuf.at[qk[k], :, columns(s)], pbuf.at[i, qk[k]],
            p_send.at[i, qk[k]], p_recv.at[i, qk[k]], partner,
        )

    def scopy(s, k):
        i = lax.rem(s, 2)
        return rcopy(
            xbuf.at[qk[k], :, columns(s)], rbuf.at[i, k - 1],
            r_send.at[i, k - 1], r_recv.at[i, k - 1], at(k),
        )

    def finish(s, k):
        @pl.when(lax.div(s, 2) == c)
        def _():
            pcopy(s, k).wait_recv()

            def step(m, _):
                here = pl.ds(pl.multiple_of(m * tile, 16), tile)
                both = xbuf[qk[k], here, columns(s)].astype(jnp.float32) + pbuf[
                    lax.rem(s, 2), qk[k], here, :
                ].astype(jnp.float32)
                xbuf[qk[k], here, columns(s)] = both.astype(jnp.bfloat16)
                return 0

            lax.fori_loop(0, tiles, step, 0)
            if k:
                scopy(s, k).start()

    def down(t):
        s = turn(t)
        for n, k in enumerate(order):
            def step(m, _):
                here = pl.ds(pl.multiple_of(m * tile, 16), tile)
                h = hid[pl.ds(pl.multiple_of(qk[k] * rows + m * tile, 16), tile), :]
                w = jnp.concatenate([wd[4 * s + j] for j in range(4)], axis=1)
                o = lax.dot_general(h, w, NN, preferred_element_type=jnp.float32)
                xbuf[qk[k], here, columns(s)] = o.astype(jnp.bfloat16)
                return 0

            lax.fori_loop(0, tiles, step, 0)
            pl.when(lax.div(s, 2) != c)(lambda: pcopy(s, k).start())
            if n:
                finish(s, order[n - 1])
        finish(s, order[-1])

    down(0)
    down(1)
    down(2)
    relay(1, 3)
    down(3)

    for i in range(2):
        s = 2 * c + i
        for k in (1, 2, 3):
            scopy(s, k).wait_recv()

        def step(m, _):
            here = pl.ds(pl.multiple_of(m * tile, 16), tile)
            total = xbuf[q, here, columns(s)].astype(jnp.float32)
            for k in range(3):
                total = total + rbuf[i, k, here, :].astype(jnp.float32)
            cols = slice(i * width, (i + 1) * width)
            out_ref[here, cols] = (total * ds_ref[:, cols]).astype(jnp.bfloat16)
            return 0

        lax.fori_loop(0, tiles, step, 0)

    for cls in (0, 1):
        for k in (1, 2, 3):
            rsh(cls, k, f).wait_send()
        for r in range(3):
            for k in range(4):
                low, high = 4 * (z - r) + qk[k], 4 * (z + r) + qk[k]
                pl.when((z >= r) & (z < 3))(lambda: zcopy(cls, low, 0).wait_send())
                pl.when((z + r <= 3) & (z > 0))(lambda: zcopy(cls, high, 1).wait_send())
    for k in (1, 2):
        for p in (0, 1):
            xcopy(k, p, q).wait_send()
    for i in range(2):
        for k in range(4):
            pcopy(2 * (1 - c) + i, k).wait_send()
            if k:
                scopy(2 * c + i, k).wait_send()


def planes(tokens, norm_gain, gate_weight, up_weight, gate_scale, up_scale, down_weight, down_scale):
    rows, model = tokens.shape
    block, units = gate_weight.shape
    part, width = units // 4, 4 * block
    normed = norm(tokens, norm_gain)
    gu = jnp.stack([gate_weight.astype(jnp.bfloat16).T, up_weight.astype(jnp.bfloat16).T])
    low = down_weight.astype(jnp.bfloat16)
    first = lax.rem(lax.axis_index("fs"), 4) * part
    gs = lax.dynamic_slice(gate_scale, (first,), (part,))[None]
    us = lax.dynamic_slice(up_scale, (first,), (part,))[None]
    bf, f32, dma = jnp.bfloat16, jnp.float32, pltpu.SemaphoreType.DMA
    hbm = pl.BlockSpec(memory_space=pl.ANY)
    vmem = pl.BlockSpec(memory_space=pltpu.VMEM)
    return pl.pallas_call(
        kernel,
        out_shape=jax.ShapeDtypeStruct((rows, down_scale.shape[0]), bf),
        in_specs=[hbm, hbm, hbm, vmem, vmem, vmem],
        out_specs=vmem,
        scratch_shapes=[
            pltpu.VMEM((4, rows, model), bf),
            pltpu.VMEM((16, 2, part, block), bf),
            pltpu.VMEM((16, part, block), bf),
            pltpu.VMEM((4 * rows, part), f32),
            pltpu.VMEM((4 * rows, part), f32),
            pltpu.VMEM((4 * rows, part), bf),
            pltpu.VMEM((2, 4, rows, width), bf),
            pltpu.VMEM((2, 3, rows, width), bf),
            dma((2,)), dma, dma((2, 3)), dma((2, 3)),
            dma((2, 2)), dma((2, 2)), dma((2,)), dma((2,)), dma((3, 2)), dma((3, 2)),
            dma((2, 2, 16)), dma((2, 16)),
            dma((2, 4)), dma((2, 4)), dma((2, 3)), dma((2, 3)),
        ],
        compiler_params=pltpu.CompilerParams(
            collective_id=0, has_side_effects=True, vmem_limit_bytes=67043328
        ),
    )(gu, low, normed, gs, us, down_scale[None])


def solution(mesh):
    in_specs = (
        P("fs", None),
        P(),
        P("fs", "tp"),
        P("fs", "tp"),
        P("tp"),
        P("tp"),
        P("tp", "fs"),
        P("tp"),
    )
    out_specs = P("fs", "tp")
    body = planes if (mesh.shape["fs"], mesh.shape["tp"]) == (16, 2) else gathered
    return jax.shard_map(body, mesh=mesh, in_specs=in_specs, out_specs=out_specs, check_vma=False)
```
